32 devices in a mesh: sp: 8 (over z, x), tp: 4 (over y, core).
Axes of the slice: x: 2, y: 2, z: 4, core: 2. Of those that a mesh axis runs over, the one named last changes fastest.
Arguments:
- prompt_tokens: bfloat16 [8192, 2048], P(('sp', 'tp')), may hold values from -8 to 8
- key_weight: bfloat16 [2048, 2048], P(None, 'tp'), may hold values from -0.125 to 0.125
- value_weight: bfloat16 [2048, 4096], P(None, 'tp'), may hold values from -0.125 to 0.125
- input_weight: bfloat16 [2048, 32], replicated, may hold values from -4 to 4
- forget_weight: bfloat16 [2048, 32], replicated, may hold values from -0.125 to 0.125
- forget_bias: float32 [32], replicated, as said below
- new_token: bfloat16 [2048], replicated, may hold values from -8 to 8
- new_query: bfloat16 [2048], P('tp'), may hold values from -6 to 6
Outputs:
- key_cache: bfloat16 [8192, 2048], P('sp', 'tp')
- value_cache: bfloat16 [8192, 4096], P('sp', 'tp')
- cache_weight: float32 [32, 8192], P('tp', 'sp')
- reading: float32 [4096], P('tp')
The draws below stay inside these ranges and needn't reach their ends.
Inputs may be any that keep to these rules, and one draw needn't show every extreme that they name: `forget_bias`: every head's forget gate offset is 2 or more.
All inputs are finite; a program needn't handle non-finite values.
Results may differ from the reference program's by a relative error of at most 0.0058.
Values may be sent and summed in bfloat16 or wider, within the bound.
A program may use at most 64 MiB of HBM per device.

```python
import math
import jax
import jax.numpy as jnp
from jax import lax

D = 2048
H = 32
DQK = 64
DV = 128
LEN = 8192


def draw_prompt_tokens(key, part):
    base_key = jax.random.fold_in(key, 11)
    scale_key = jax.random.fold_in(key, 12)
    base_draw = jnp.clip(jax.random.normal(base_key, (LEN, D), jnp.float32), -5.0, 5.0)
    block_count = LEN // 32
    block_scales = jnp.exp(jax.random.uniform(scale_key, (block_count, 1), jnp.float32, math.log(0.5), math.log(1.6)))
    block_scales = jnp.repeat(block_scales, 32, axis=0)
    return (base_draw * block_scales).astype(jnp.bfloat16)


def draw_input_weight(key, part):
    base_draw = jnp.clip(jax.random.normal(jax.random.fold_in(key, 21), (D, H), jnp.float32), -4.0, 4.0) * D ** (-0.5)
    return base_draw.astype(jnp.bfloat16)


def draw_forget_bias(key, part):
    picked = jax.random.uniform(jax.random.fold_in(key, 31), (H,), jnp.float32)
    quick_rates = jax.random.uniform(jax.random.fold_in(key, 32), (H,), jnp.float32, 3.0, 4.5)
    slow_rates = math.log(LEN) + jax.random.uniform(jax.random.fold_in(key, 33), (H,), jnp.float32, 0.0, 1.5)
    quick_share = 0.5
    return jnp.where(picked < quick_share, quick_rates, slow_rates)


def level_of(key, dims, split, low, largest):
    factor_of, own = 1.0, jax.random.fold_in(key, 6)
    for axis_at, shards_of in split:
        steps = jnp.exp(jax.random.uniform(jax.random.fold_in(own, axis_at), (shards_of,), jnp.float32, low / len(split), largest / len(split)))
        factor_of = factor_of * jnp.repeat(steps, dims[axis_at] // shards_of).reshape([-1 if axis == axis_at else 1 for axis in range(len(dims))])
    return factor_of


def centred(own_key, extent, spread, limit, pieces=(), kind=jnp.bfloat16):
    factor_of = level_of(own_key, extent, pieces, -0.22, 0.18) if pieces else 1.0
    drawn = jax.random.normal(own_key, extent, jnp.float32) * spread * factor_of
    return jnp.minimum(jnp.maximum(drawn, -limit), limit).astype(kind)


def setup_inputs(seed: int = 0) -> dict:
    streams_of = jax.random.split(jax.random.key(seed), 9)
    prompt_tokens = draw_prompt_tokens(jax.random.fold_in(streams_of[8], 71), 0)
    key_weight = centred(streams_of[1], (D, H * DQK), D ** -0.5, 0.125, ((1, 4),))
    value_weight = centred(streams_of[2], (D, H * DV), D ** -0.5, 0.125, ((1, 4),))
    input_weight = draw_input_weight(jax.random.fold_in(streams_of[8], 71), 0)
    forget_weight = centred(streams_of[4], (D, H), D ** -0.5, 0.125)
    forget_bias = draw_forget_bias(jax.random.fold_in(streams_of[8], 71), 0)
    new_token = centred(streams_of[6], (D,), 2.0, 8.0)
    new_query = centred(streams_of[7], (H * DQK,), 1.0, 6.0, ((0, 4),))
    return {"prompt_tokens": prompt_tokens, "key_weight": key_weight, "value_weight": value_weight, "input_weight": input_weight, "forget_weight": forget_weight, "forget_bias": forget_bias, "new_token": new_token, "new_query": new_query}


def reference(prompt_tokens, key_weight, value_weight, input_weight, forget_weight, forget_bias, new_token, new_query):
    key_cache = jnp.dot(prompt_tokens, key_weight, preferred_element_type=jnp.float32).astype(jnp.bfloat16)
    value_cache = jnp.dot(prompt_tokens, value_weight, preferred_element_type=jnp.float32).astype(jnp.bfloat16)
    input_gate = jnp.dot(prompt_tokens, input_weight, preferred_element_type=jnp.float32)
    log_forget = jax.nn.log_sigmoid(jnp.dot(prompt_tokens, forget_weight, preferred_element_type=jnp.float32) + forget_bias)
    log_weight = input_gate + (lax.optimization_barrier(jnp.sum(log_forget, axis=0, keepdims=True)) - jnp.cumsum(log_forget, axis=0))
    peak_log = lax.optimization_barrier(jnp.max(log_weight, axis=0))
    cache_weight = jnp.transpose(jnp.exp(log_weight - peak_log[None, :]), (1, 0))
    new_key = jnp.dot(new_token, key_weight, preferred_element_type=jnp.float32).astype(jnp.bfloat16)
    new_value = jnp.dot(new_token, value_weight, preferred_element_type=jnp.float32).astype(jnp.bfloat16)
    new_gate = jnp.dot(new_token, input_weight, preferred_element_type=jnp.float32)
    new_forget = jax.nn.log_sigmoid(jnp.dot(new_token, forget_weight, preferred_element_type=jnp.float32) + forget_bias)
    stable_level = jnp.maximum(new_forget + peak_log, new_gate)
    query_heads = new_query.astype(jnp.float32).reshape(H, DQK)
    key_heads = key_cache.astype(jnp.float32).reshape(LEN, H, DQK)
    key_score = jnp.einsum('shd,hd->sh', key_heads, query_heads, precision=lax.Precision.HIGHEST) / math.sqrt(DQK)
    new_heads = new_key.astype(jnp.float32).reshape(H, DQK)
    new_score = jnp.einsum('hd,hd->h', new_heads, query_heads, precision=lax.Precision.HIGHEST) / math.sqrt(DQK)
    weighted = jnp.exp(new_forget[None, :] + log_weight - stable_level[None, :]) * key_score
    weighted_low = weighted.astype(jnp.bfloat16)
    own_term = jnp.exp(new_gate - stable_level) * new_score
    value_heads = value_cache.astype(jnp.float32).reshape(LEN, H, DV)
    numerator = jnp.einsum('sh,she->he', weighted_low.astype(jnp.float32), value_heads, precision=lax.Precision.HIGHEST)
    numerator = numerator + own_term[:, None] * new_value.astype(jnp.float32).reshape(H, DV)
    denominator = lax.optimization_barrier(jnp.sum(weighted, axis=0)) + own_term
    reading = numerator / jnp.maximum(jnp.abs(denominator), 1.0)[:, None]
    return (key_cache, value_cache, cache_weight, reading.reshape(H * DV))
```

```python
import functools
import math

import jax
import jax.numpy as jnp
from jax import lax
from jax.experimental import pallas as pl
from jax.experimental.pallas import tpu as pltpu
from jax.sharding import PartitionSpec as P

DQK = 64
DV = 128
PAD = 16
MESH = pl.DeviceIdType.MESH
NT = (((1,), (1,)), ((), ()))


def dot(a, b):
    return jnp.dot(a, b, preferred_element_type=jnp.float32)


def dot_nt(a, b):
    return lax.dot_general(a, b, NT, preferred_element_type=jnp.float32)


def log_sigmoid(x):
    return jnp.minimum(x, 0.0) - jnp.log1p(jnp.exp(-jnp.abs(x)))


def pieces_of(rows):
    return [(0, rows // 2), (rows // 2, rows // 4), (rows // 2 + rows // 4, rows // 4)]


def kernel(
    n_sp,
    n_tp,
    tok_hbm,
    kw_hbm,
    vw_hbm,
    wi_ref,
    wf_ref,
    fb_ref,
    nt_ref,
    nq_ref,
    k_out,
    v_out,
    cw_out,
    rd_out,
    tok,
    kw,
    vw,
    gnew,
    s1_src,
    s1,
    s2_src,
    s2,
    s3_src,
    s3,
    lwb,
    wexp,
    local_sem,
    near_sem,
    far_send,
    far_recv,
    fwd_send,
    fwd_recv,
    s1_send,
    s1_recv,
    s2_send,
    s2_recv,
    s3_send,
    s3_recv,
):
    sp, tp = lax.axis_index("sp"), lax.axis_index("tp")
    chips = n_tp // 2
    chip, core = tp // 2, tp % 2
    mate = chip * 2 + (1 - core)
    rows = tok.shape[1]
    heads = s2_src.shape[0]
    all_heads = wi_ref.shape[0]
    pieces = pieces_of(rows)

    load_tok = pltpu.make_async_copy(tok_hbm, tok.at[tp], local_sem.at[0])
    load_kw = pltpu.make_async_copy(kw_hbm, kw, local_sem.at[1])
    load_vw = pltpu.make_async_copy(vw_hbm, vw, local_sem.at[2])
    load_tok.start()
    load_kw.start()
    load_vw.start()

    barrier = pltpu.get_barrier_semaphore()
    for k in range(1, n_tp):
        pl.semaphore_signal(
            barrier, inc=1, device_id=(sp, (tp + k) % n_tp), device_id_type=MESH
        )
    for k in range(1, n_sp):
        pl.semaphore_signal(
            barrier, inc=1, device_id=((sp + k) % n_sp, tp), device_id_type=MESH
        )
    pl.semaphore_wait(barrier, n_tp - 1 + n_sp - 1)

    def remote(src, dst, send, recv, device):
        return pltpu.make_async_remote_copy(
            src_ref=src,
            dst_ref=dst,
            send_sem=send,
            recv_sem=recv,
            device_id=device,
            device_id_type=MESH,
        )

    def far_copy(k, j):
        at, size = pieces[j]
        there = ((chip + k) % chips) * 2 + core
        return remote(
            tok_hbm.at[pl.ds(at, size)],
            tok.at[tp, pl.ds(at, size)],
            far_send.at[k - 1, j],
            far_recv.at[k - 1, j],
            (sp, there),
        )

    def came_from(k):
        return (chip - k + chips) % chips

    def forward_copy(k, j):
        at, size = pieces[j]
        slot = came_from(k) * 2 + core
        return remote(
            tok.at[slot, pl.ds(at, size)],
            tok.at[slot, pl.ds(at, size)],
            fwd_send.at[k - 1, j],
            fwd_recv.at[k - 1, j],
            (sp, mate),
        )

    near = remote(tok_hbm, tok.at[tp], near_sem.at[0], near_sem.at[1], (sp, mate))
    for k in range(1, chips):
        far_copy(k, 0).start()
    near.start()

    row_iota = lax.broadcasted_iota(jnp.int32, (all_heads, all_heads), 0)
    col_iota = lax.broadcasted_iota(jnp.int32, (all_heads, all_heads), 1)
    shift = jnp.sum(jnp.where(row_iota == col_iota, fb_ref[...], 0.0), axis=1, keepdims=True)
    load_tok.wait()
    own = tok[tp]
    gate = dot_nt(wi_ref[...], own)
    log_forget = log_sigmoid(dot_nt(wf_ref[...], own) + shift)
    later = lax.broadcasted_iota(jnp.int32, (rows, rows), 0) > lax.broadcasted_iota(
        jnp.int32, (rows, rows), 1
    )
    decay = jnp.dot(
        log_forget,
        later.astype(jnp.float32),
        precision=lax.Precision.HIGHEST,
        preferred_element_type=jnp.float32,
    )
    relative = gate + decay
    total = jnp.broadcast_to(jnp.sum(log_forget, axis=1, keepdims=True), (all_heads, 128))
    for t in range(n_tp):
        part = slice(t * heads, (t + 1) * heads)
        s1_src[t, :, :rows] = relative[part]
        s1_src[t, :, rows:] = total[part]

    def s1_copy(k):
        there = (tp + k) % n_tp
        return remote(
            s1_src.at[there], s1.at[tp], s1_send.at[k - 1], s1_recv.at[k - 1], (sp, there)
        )

    for k in range(1, n_tp):
        s1_copy(k).start()
    s1[tp] = s1_src[tp]
    for j in range(1, len(pieces)):
        for k in range(1, chips):
            far_copy(k, j).start()

    fresh = nt_ref[...]
    new_gates = dot_nt(wi_ref[...], fresh)[:, :1]
    new_forgets = log_sigmoid(dot_nt(wf_ref[...], fresh)[:, :1] + shift)
    for t in range(n_tp):
        part = slice(t * heads, (t + 1) * heads)
        gnew[t, :, :128] = jnp.broadcast_to(new_gates[part], (heads, 128))
        gnew[t, :, 128:] = jnp.broadcast_to(new_forgets[part], (heads, 128))

    def product(slot, at, size):
        first = pl.multiple_of(slot * rows + at, PAD)
        for w, out in ((kw, k_out), (vw, v_out)):
            wide = min(256, w.shape[1])

            @pl.loop(0, w.shape[1] // wide)
            def _(c):
                cols = pl.ds(pl.multiple_of(c * wide, wide), wide)
                out[pl.ds(first, size), cols] = dot(
                    tok[slot, pl.ds(at, size)], w[:, cols]
                ).astype(jnp.bfloat16)

    load_kw.wait()
    load_vw.wait()
    product(tp, 0, rows)

    for k in range(1, n_tp):
        s1_copy(k).wait_recv()
    run = jnp.zeros((heads, 1), jnp.float32)
    top = jnp.full((heads, 1), -jnp.inf, jnp.float32)
    for t in reversed(range(n_tp)):
        here = s1[t, :, :rows] + run
        lwb[t] = here
        top = jnp.maximum(top, jnp.max(here, axis=1, keepdims=True))
        run = run + s1[t, :, rows : rows + 1]
    lane = lax.broadcasted_iota(jnp.int32, (heads, 128), 1)
    s2_src[...] = jnp.where(lane < 64, run, top)

    def s2_copy(k):
        return remote(
            s2_src, s2.at[sp], s2_send.at[k - 1], s2_recv.at[k - 1], ((sp + k) % n_sp, tp)
        )

    for k in range(1, n_sp):
        s2_copy(k).start()
    s2[sp] = s2_src[...]

    near.wait_recv()
    product(mate, 0, rows)

    for k in range(1, n_sp):
        s2_copy(k).wait_recv()
    run = jnp.zeros((heads, 1), jnp.float32)
    carried = jnp.zeros((heads, 1), jnp.float32)
    peak = jnp.full((heads, 1), -jnp.inf, jnp.float32)
    for b in reversed(range(n_sp)):
        peak = jnp.maximum(peak, s2[b, :, 64:65] + run)
        carried = jnp.where(b == sp, run, carried)
        run = run + s2[b, :, 0:1]
    new_gate = gnew[tp, :, 0:1]
    new_forget = gnew[tp, :, 128:129]
    stable = jnp.maximum(new_forget + peak, new_gate)
    for t in range(n_tp):
        log_weight = lwb[t] + carried
        cw_out[:, t * rows : (t + 1) * rows] = jnp.exp(log_weight - peak)
        wexp[t] = jnp.exp(new_forget + log_weight - stable)

    scale = 1.0 / math.sqrt(DQK)
    key_cols, value_cols = kw.shape[1], vw.shape[1]
    owner = lax.broadcasted_iota(jnp.int32, (heads, key_cols), 1) // DQK
    head = lax.broadcasted_iota(jnp.int32, (heads, key_cols), 0)
    query = jnp.where(
        owner == head, jnp.broadcast_to(nq_ref[...].astype(jnp.float32), (heads, key_cols)), 0.0
    )
    query_low = query.astype(jnp.bfloat16)
    which = lax.broadcasted_iota(jnp.int32, (heads, DV), 0)

    def own_columns(wide):
        found = jnp.zeros((heads, DV), jnp.float32)
        for h in range(heads):
            found = found + jnp.where(which == h, wide[:, h * DV : (h + 1) * DV], 0.0)
        return found

    new_key = dot(fresh, kw[...])[:1].astype(jnp.bfloat16).astype(jnp.float32)
    new_score = jnp.sum(query * new_key, axis=1, keepdims=True) * scale
    new_value = dot(fresh, vw[...])[:heads].astype(jnp.bfloat16).astype(jnp.float32)
    own_term = jnp.exp(new_gate - stable) * new_score
    own_value = own_term * own_columns(new_value)

    numer = jnp.zeros((heads, value_cols), jnp.float32)
    denom = jnp.zeros((heads, 1), jnp.float32)

    def read(slot, at, size, numer, denom):
        first = pl.multiple_of(slot * rows + at, PAD)
        score = dot_nt(query_low, k_out[pl.ds(first, size)]) * scale
        weighted = wexp[slot, :, at : at + size] * score
        numer = numer + dot(weighted.astype(jnp.bfloat16), v_out[pl.ds(first, size)])
        return numer, denom + jnp.sum(weighted, axis=1, keepdims=True)

    numer, denom = read(tp, 0, rows, numer, denom)
    numer, denom = read(mate, 0, rows, numer, denom)

    last = len(pieces) - 1
    for j, (at, size) in enumerate(pieces):
        for k in range(1, chips):
            far_copy(k, j).wait_recv()
            forward_copy(k, j).start()
            product(came_from(k) * 2 + core, at, size)
        for k in range(1, chips):
            forward_copy(k, j).wait_recv()
            product(came_from(k) * 2 + 1 - core, at, size)
        if j == 0 or j == last:
            start, count = (0, rows // 2) if j == 0 else (rows // 2, rows // 2)
            for k in range(1, chips):
                for side in (core, 1 - core):
                    numer, denom = read(came_from(k) * 2 + side, start, count, numer, denom)

    s3_src[:, :DV] = own_columns(numer)
    s3_src[:, DV:] = jnp.broadcast_to(denom, (heads, 128))

    def s3_copy(k):
        return remote(
            s3_src, s3.at[sp], s3_send.at[k - 1], s3_recv.at[k - 1], ((sp + k) % n_sp, tp)
        )

    for k in range(1, n_sp):
        s3_copy(k).start()
    s3[sp] = s3_src[...]
    near.wait_send()
    for j in range(len(pieces)):
        for k in range(1, chips):
            far_copy(k, j).wait_send()
            forward_copy(k, j).wait_send()
    for k in range(1, n_tp):
        s1_copy(k).wait_send()
    for k in range(1, n_sp):
        s2_copy(k).wait_send()
    for k in range(1, n_sp):
        s3_copy(k).wait_recv()
    gathered = s3[0]
    for b in range(1, n_sp):
        gathered = gathered + s3[b]
    numerator = gathered[:, :DV] + own_value
    denominator = gathered[:, DV : DV + 1] + own_term
    rd_out[...] = numerator / jnp.maximum(jnp.abs(denominator), 1.0)
    for k in range(1, n_sp):
        s3_copy(k).wait_send()


def body(
    n_sp,
    n_tp,
    prompt_tokens,
    key_weight,
    value_weight,
    input_weight,
    forget_weight,
    forget_bias,
    new_token,
    new_query,
):
    rows, depth = prompt_tokens.shape
    key_cols, value_cols = key_weight.shape[1], value_weight.shape[1]
    heads = key_cols // DQK
    block = rows * n_tp
    steps = len(pieces_of(rows))
    chips = n_tp // 2
    vmem = pl.BlockSpec(memory_space=pltpu.VMEM)
    hbm = pl.BlockSpec(memory_space=pl.ANY)
    dma = pltpu.SemaphoreType.DMA
    f32, bf16 = jnp.float32, jnp.bfloat16
    keys, values, weights, reading = pl.pallas_call(
        functools.partial(kernel, n_sp, n_tp),
        out_shape=(
            jax.ShapeDtypeStruct((block, key_cols), bf16),
            jax.ShapeDtypeStruct((block, value_cols), bf16),
            jax.ShapeDtypeStruct((heads, block), f32),
            jax.ShapeDtypeStruct((heads, DV), f32),
        ),
        in_specs=[hbm] * 3 + [vmem] * 5,
        out_specs=(vmem,) * 4,
        scratch_shapes=[
            pltpu.VMEM((n_tp, rows, depth), bf16),
            pltpu.VMEM((depth, key_cols), bf16),
            pltpu.VMEM((depth, value_cols), bf16),
            pltpu.VMEM((n_tp, heads, 256), f32),
            pltpu.VMEM((n_tp, heads, rows + 128), f32),
            pltpu.VMEM((n_tp, heads, rows + 128), f32),
            pltpu.VMEM((heads, 128), f32),
            pltpu.VMEM((n_sp, heads, 128), f32),
            pltpu.VMEM((heads, DV + 128), f32),
            pltpu.VMEM((n_sp, heads, DV + 128), f32),
            pltpu.VMEM((n_tp, heads, rows), f32),
            pltpu.VMEM((n_tp, heads, rows), f32),
            dma((3,)),
            dma((2,)),
            dma((chips - 1, steps)),
            dma((chips - 1, steps)),
            dma((chips - 1, steps)),
            dma((chips - 1, steps)),
            dma((n_tp - 1,)),
            dma((n_tp - 1,)),
            dma((n_sp - 1,)),
            dma((n_sp - 1,)),
            dma((n_sp - 1,)),
            dma((n_sp - 1,)),
        ],
        compiler_params=pltpu.CompilerParams(collective_id=0, has_side_effects=True),
    )(
        prompt_tokens,
        key_weight,
        value_weight,
        input_weight.T,
        forget_weight.T,
        forget_bias[None, :],
        jnp.broadcast_to(new_token[None, :], (PAD, depth)),
        new_query[None, :],
    )
    return keys, values, weights, reading.reshape(-1)


def solution(mesh):
    placed = (P(("sp", "tp"), None), P(None, "tp"), P(None, "tp"), P(), P(), P(), P(), P("tp"))
    return jax.shard_map(
        functools.partial(body, mesh.shape["sp"], mesh.shape["tp"]),
        mesh=mesh,
        in_specs=placed,
        out_specs=(P("sp", "tp"), P("sp", "tp"), P("tp", "sp"), P("tp")),
        check_vma=False,
    )
```

```python
import functools
import math

import jax
import jax.numpy as jnp
from jax import lax
from jax.experimental import pallas as pl
from jax.experimental.pallas import tpu as pltpu
from jax.sharding import PartitionSpec as P

DQK = 64
DV = 128
PAD = 16
MESH = pl.DeviceIdType.MESH
NT = (((1,), (1,)), ((), ()))


def dot(a, b):
    return jnp.dot(a, b, preferred_element_type=jnp.float32)


def dot_nt(a, b):
    return lax.dot_general(a, b, NT, preferred_element_type=jnp.float32)


def log_sigmoid(x):
    return jnp.minimum(x, 0.0) - jnp.log1p(jnp.exp(-jnp.abs(x)))


def pieces_of(rows):
    return [(0, rows // 2), (rows // 2, rows // 4), (rows // 2 + rows // 4, rows // 4)]


def kernel(
    n_sp,
    n_tp,
    tok_hbm,
    kw_hbm,
    vw_hbm,
    wi_hbm,
    wf_hbm,
    fb_hbm,
    nt_hbm,
    nq_hbm,
    k_out,
    v_out,
    cw_out,
    rd_out,
    tok,
    kw,
    vw,
    wi_ref,
    wf_ref,
    fb_ref,
    nt_ref,
    nq_ref,
    gnew,
    s1_src,
    s1,
    s2_src,
    s2,
    s3_src,
    s3,
    lwb,
    wexp,
    local_sem,
    near_sem,
    far_send,
    far_recv,
    fwd_send,
    fwd_recv,
    s1_send,
    s1_recv,
    s2_send,
    s2_recv,
    s3_send,
    s3_recv,
):
    sp, tp = lax.axis_index("sp"), lax.axis_index("tp")
    chips = n_tp // 2
    chip, core = tp // 2, tp % 2
    mate = chip * 2 + (1 - core)
    rows = tok.shape[1]
    heads = s2_src.shape[0]
    all_heads = wi_ref.shape[0]
    pieces = pieces_of(rows)

    barrier = pltpu.get_barrier_semaphore()
    for k in range(1, n_tp):
        pl.semaphore_signal(
            barrier, inc=1, device_id=(sp, (tp + k) % n_tp), device_id_type=MESH
        )
    for k in range(1, n_sp):
        pl.semaphore_signal(
            barrier, inc=1, device_id=((sp + k) % n_sp, tp), device_id_type=MESH
        )
    loads = [
        pltpu.make_async_copy(src, dst, local_sem.at[i])
        for i, (src, dst) in enumerate(
            (
                (tok_hbm, tok.at[tp]),
                (wi_hbm, wi_ref),
                (wf_hbm, wf_ref),
                (fb_hbm, fb_ref),
                (nt_hbm, nt_ref),
                (nq_hbm, nq_ref),
                (kw_hbm, kw),
                (vw_hbm, vw),
            )
        )
    ]
    for load in loads:
        load.start()
    pl.semaphore_wait(barrier, n_tp - 1 + n_sp - 1)

    def remote(src, dst, send, recv, device):
        return pltpu.make_async_remote_copy(
            src_ref=src,
            dst_ref=dst,
            send_sem=send,
            recv_sem=recv,
            device_id=device,
            device_id_type=MESH,
        )

    def far_copy(k, j):
        at, size = pieces[j]
        there = ((chip + k) % chips) * 2 + core
        return remote(
            tok_hbm.at[pl.ds(at, size)],
            tok.at[tp, pl.ds(at, size)],
            far_send.at[k - 1, j],
            far_recv.at[k - 1, j],
            (sp, there),
        )

    def came_from(k):
        return (chip - k + chips) % chips

    def forward_copy(k, j):
        at, size = pieces[j]
        slot = came_from(k) * 2 + core
        return remote(
            tok.at[slot, pl.ds(at, size)],
            tok.at[slot, pl.ds(at, size)],
            fwd_send.at[k - 1, j],
            fwd_recv.at[k - 1, j],
            (sp, mate),
        )

    near = remote(tok_hbm, tok.at[tp], near_sem.at[0], near_sem.at[1], (sp, mate))
    for k in range(1, chips):
        far_copy(k, 0).start()
    near.start()

    for load in loads[:6]:
        load.wait()
    row_iota = lax.broadcasted_iota(jnp.int32, (all_heads, all_heads), 0)
    col_iota = lax.broadcasted_iota(jnp.int32, (all_heads, all_heads), 1)
    shift = jnp.sum(jnp.where(row_iota == col_iota, fb_ref[...], 0.0), axis=1, keepdims=True)
    own = tok[tp]
    gate = dot_nt(wi_ref[...], own)
    log_forget = log_sigmoid(dot_nt(wf_ref[...], own) + shift)
    later = lax.broadcasted_iota(jnp.int32, (rows, rows), 0) > lax.broadcasted_iota(
        jnp.int32, (rows, rows), 1
    )
    decay = jnp.dot(
        log_forget,
        later.astype(jnp.float32),
        precision=lax.Precision.HIGHEST,
        preferred_element_type=jnp.float32,
    )
    relative = gate + decay
    total = jnp.broadcast_to(jnp.sum(log_forget, axis=1, keepdims=True), (all_heads, 128))
    for t in range(n_tp):
        part = slice(t * heads, (t + 1) * heads)
        s1_src[t, :, :rows] = relative[part]
        s1_src[t, :, rows:] = total[part]

    def s1_copy(k):
        there = (tp + k) % n_tp
        return remote(
            s1_src.at[there], s1.at[tp], s1_send.at[k - 1], s1_recv.at[k - 1], (sp, there)
        )

    for k in range(1, n_tp):
        s1_copy(k).start()
    s1[tp] = s1_src[tp]
    for j in range(1, len(pieces)):
        for k in range(1, chips):
            far_copy(k, j).start()

    fresh = jnp.broadcast_to(nt_ref[...].reshape(1, -1), (PAD, nt_ref.shape[0]))
    new_gates = dot_nt(wi_ref[...], fresh)[:, :1]
    new_forgets = log_sigmoid(dot_nt(wf_ref[...], fresh)[:, :1] + shift)
    for t in range(n_tp):
        part = slice(t * heads, (t + 1) * heads)
        gnew[t, :, :128] = jnp.broadcast_to(new_gates[part], (heads, 128))
        gnew[t, :, 128:] = jnp.broadcast_to(new_forgets[part], (heads, 128))

    def product(slot, at, size):
        first = pl.multiple_of(slot * rows + at, PAD)
        for w, out in ((kw, k_out), (vw, v_out)):
            wide = min(256, w.shape[1])

            def tile(c):
                cols = pl.ds(pl.multiple_of(c * wide, wide), wide)
                out[pl.ds(first, size), cols] = dot(
                    tok[slot, pl.ds(at, size)], w[:, cols]
                ).astype(jnp.bfloat16)

            if size <= 64:
                out[pl.ds(first, size), :] = dot(
                    tok[slot, pl.ds(at, size)], w[...]
                ).astype(jnp.bfloat16)
            else:
                pl.loop(0, w.shape[1] // wide)(tile)

    for load in loads[6:]:
        load.wait()
    product(tp, 0, rows)

    for k in range(1, n_tp):
        s1_copy(k).wait_recv()
    run = jnp.zeros((heads, 1), jnp.float32)
    top = jnp.full((heads, 1), -jnp.inf, jnp.float32)
    for t in reversed(range(n_tp)):
        here = s1[t, :, :rows] + run
        lwb[t] = here
        top = jnp.maximum(top, jnp.max(here, axis=1, keepdims=True))
        run = run + s1[t, :, rows : rows + 1]
    lane = lax.broadcasted_iota(jnp.int32, (heads, 128), 1)
    s2_src[...] = jnp.where(lane < 64, run, top)

    def s2_copy(k):
        return remote(
            s2_src, s2.at[sp], s2_send.at[k - 1], s2_recv.at[k - 1], ((sp + k) % n_sp, tp)
        )

    for k in range(1, n_sp):
        s2_copy(k).start()
    s2[sp] = s2_src[...]

    near.wait_recv()
    product(mate, 0, rows)

    for k in range(1, n_sp):
        s2_copy(k).wait_recv()
    run = jnp.zeros((heads, 1), jnp.float32)
    carried = jnp.zeros((heads, 1), jnp.float32)
    peak = jnp.full((heads, 1), -jnp.inf, jnp.float32)
    for b in reversed(range(n_sp)):
        peak = jnp.maximum(peak, s2[b, :, 64:65] + run)
        carried = jnp.where(b == sp, run, carried)
        run = run + s2[b, :, 0:1]
    new_gate = gnew[tp, :, 0:1]
    new_forget = gnew[tp, :, 128:129]
    stable = jnp.maximum(new_forget + peak, new_gate)
    for t in range(n_tp):
        log_weight = lwb[t] + carried
        cw_out[:, t * rows : (t + 1) * rows] = jnp.exp(log_weight - peak)
        wexp[t] = jnp.exp(new_forget + log_weight - stable)

    scale = 1.0 / math.sqrt(DQK)
    key_cols, value_cols = kw.shape[1], vw.shape[1]
    owner = lax.broadcasted_iota(jnp.int32, (heads, key_cols), 1) // DQK
    head = lax.broadcasted_iota(jnp.int32, (heads, key_cols), 0)
    query = jnp.where(
        owner == head, jnp.broadcast_to(nq_ref[...].reshape(1, -1).astype(jnp.float32), (heads, key_cols)), 0.0
    )
    query_low = query.astype(jnp.bfloat16)
    which = lax.broadcasted_iota(jnp.int32, (heads, DV), 0)

    def own_columns(wide):
        found = jnp.zeros((heads, DV), jnp.float32)
        for h in range(heads):
            found = found + jnp.where(which == h, wide[:, h * DV : (h + 1) * DV], 0.0)
        return found

    new_key = dot(fresh, kw[...])[:1].astype(jnp.bfloat16).astype(jnp.float32)
    new_score = jnp.sum(query * new_key, axis=1, keepdims=True) * scale
    new_value = dot(fresh, vw[...])[:heads].astype(jnp.bfloat16).astype(jnp.float32)
    own_term = jnp.exp(new_gate - stable) * new_score
    own_value = own_term * own_columns(new_value)

    numer = jnp.zeros((heads, value_cols), jnp.float32)
    denom = jnp.zeros((heads, 1), jnp.float32)

    def read(slot, at, size, numer, denom):
        first = pl.multiple_of(slot * rows + at, PAD)
        score = dot_nt(query_low, k_out[pl.ds(first, size)]) * scale
        weighted = wexp[slot, :, at : at + size] * score
        numer = numer + dot(weighted.astype(jnp.bfloat16), v_out[pl.ds(first, size)])
        return numer, denom + jnp.sum(weighted, axis=1, keepdims=True)

    numer, denom = read(tp, 0, rows, numer, denom)
    numer, denom = read(mate, 0, rows, numer, denom)

    last = len(pieces) - 1
    for j, (at, size) in enumerate(pieces):
        for k in range(1, chips):
            far_copy(k, j).wait_recv()
            forward_copy(k, j).start()
            product(came_from(k) * 2 + core, at, size)
        for k in range(1, chips):
            forward_copy(k, j).wait_recv()
            product(came_from(k) * 2 + 1 - core, at, size)
        if j == 0 or j == last:
            start, count = (0, rows // 2) if j == 0 else (rows // 2, rows // 2)
            for k in range(1, chips):
                for side in (core, 1 - core):
                    numer, denom = read(came_from(k) * 2 + side, start, count, numer, denom)

    s3_src[:, :DV] = own_columns(numer)
    s3_src[:, DV:] = jnp.broadcast_to(denom, (heads, 128))

    def s3_copy(k):
        return remote(
            s3_src, s3.at[sp], s3_send.at[k - 1], s3_recv.at[k - 1], ((sp + k) % n_sp, tp)
        )

    for k in range(1, n_sp):
        s3_copy(k).start()
    s3[sp] = s3_src[...]
    near.wait_send()
    for j in range(len(pieces)):
        for k in range(1, chips):
            far_copy(k, j).wait_send()
            forward_copy(k, j).wait_send()
    for k in range(1, n_tp):
        s1_copy(k).wait_send()
    for k in range(1, n_sp):
        s2_copy(k).wait_send()
    for k in range(1, n_sp):
        s3_copy(k).wait_recv()
    gathered = s3[0]
    for b in range(1, n_sp):
        gathered = gathered + s3[b]
    numerator = gathered[:, :DV] + own_value
    denominator = gathered[:, DV : DV + 1] + own_term
    rd_out[...] = numerator / jnp.maximum(jnp.abs(denominator), 1.0)
    for k in range(1, n_sp):
        s3_copy(k).wait_send()


def body(
    n_sp,
    n_tp,
    prompt_tokens,
    key_weight,
    value_weight,
    input_weight,
    forget_weight,
    forget_bias,
    new_token,
    new_query,
):
    rows, depth = prompt_tokens.shape
    key_cols, value_cols = key_weight.shape[1], value_weight.shape[1]
    heads = key_cols // DQK
    block = rows * n_tp
    steps = len(pieces_of(rows))
    chips = n_tp // 2
    vmem = pl.BlockSpec(memory_space=pltpu.VMEM)
    hbm = pl.BlockSpec(memory_space=pl.ANY)
    dma = pltpu.SemaphoreType.DMA
    f32, bf16 = jnp.float32, jnp.bfloat16
    results = (
        ((block, key_cols), bf16),
        ((block, value_cols), bf16),
        ((heads, block), f32),
        ((heads, DV), f32),
    )
    keys, values, weights, reading = pl.pallas_call(
        functools.partial(kernel, n_sp, n_tp),
        out_shape=tuple(pltpu.VMEM(dims, kind) for dims, kind in results),
        in_specs=[hbm] * 8,
        out_specs=(vmem,) * 4,
        scratch_shapes=[
            pltpu.VMEM((n_tp, rows, depth), bf16),
            pltpu.VMEM((depth, key_cols), bf16),
            pltpu.VMEM((depth, value_cols), bf16),
            pltpu.VMEM(input_weight.shape[::-1], bf16),
            pltpu.VMEM(input_weight.shape[::-1], bf16),
            pltpu.VMEM((1,) + forget_bias.shape, f32),
            pltpu.VMEM(new_token.shape, bf16),
            pltpu.VMEM(new_query.shape, bf16),
            pltpu.VMEM((n_tp, heads, 256), f32),
            pltpu.VMEM((n_tp, heads, rows + 128), f32),
            pltpu.VMEM((n_tp, heads, rows + 128), f32),
            pltpu.VMEM((heads, 128), f32),
            pltpu.VMEM((n_sp, heads, 128), f32),
            pltpu.VMEM((heads, DV + 128), f32),
            pltpu.VMEM((n_sp, heads, DV + 128), f32),
            pltpu.VMEM((n_tp, heads, rows), f32),
            pltpu.VMEM((n_tp, heads, rows), f32),
            dma((8,)),
            dma((2,)),
            dma((chips - 1, steps)),
            dma((chips - 1, steps)),
            dma((chips - 1, steps)),
            dma((chips - 1, steps)),
            dma((n_tp - 1,)),
            dma((n_tp - 1,)),
            dma((n_sp - 1,)),
            dma((n_sp - 1,)),
            dma((n_sp - 1,)),
            dma((n_sp - 1,)),
        ],
        compiler_params=pltpu.CompilerParams(collective_id=0, has_side_effects=True),
    )(
        prompt_tokens,
        key_weight,
        value_weight,
        input_weight.T,
        forget_weight.T,
        forget_bias[None, :],
        new_token,
        new_query,
    )
    return keys, values, weights, reading.reshape(-1)


def solution(mesh):
    placed = (P(("sp", "tp"), None), P(None, "tp"), P(None, "tp"), P(), P(), P(), P(), P("tp"))
    return jax.shard_map(
        functools.partial(body, mesh.shape["sp"], mesh.shape["tp"]),
        mesh=mesh,
        in_specs=placed,
        out_specs=(P("sp", "tp"), P("sp", "tp"), P("tp", "sp"), P("tp")),
        check_vma=False,
    )
```
